32 devices in a mesh: grp: 2 (over y), ep: 8 (over z, core), tp: 2 (over x).
Axes of the slice: x: 2, y: 2, z: 4, core: 2. Of those that a mesh axis runs over, the one named last changes fastest.
Arguments:
- tokens: bfloat16 [2048, 4096], P(('grp', 'ep'), 'tp'), parts along dimension 0, may hold values from -6 to 6
- routes: int32 [2048, 4], P(('grp', 'ep')), parts along dimension 0, may hold values from 0 to 7, all different within a row; in each aligned block of 128 rows (0 to 127, 128 to 255, ...) at most 128 rows name the same one
- route_weights: float32 [2048, 4], P(('grp', 'ep')), parts along dimension 0, may hold values from 0.1 to 1
- norm_gain: float32 [4096], replicated, may hold values from 0.1 to 1.9
- expert_gate: bfloat16 [8, 4096, 1024], P('ep', 'tp'), may hold values from -0.09375 to 0.09375
- expert_up: bfloat16 [8, 4096, 1024], P('ep', 'tp'), may hold values from -0.09375 to 0.09375
- expert_down: bfloat16 [8, 1024, 4096], P('ep', None, 'tp')
- shared_gate: bfloat16 [4096, 1024], P('tp'), may hold values from -0.09375 to 0.09375
- shared_up: bfloat16 [4096, 1024], P('tp'), may hold values from -0.09375 to 0.09375
- shared_down: bfloat16 [1024, 4096], P(None, 'tp')
- out_gain: float32 [4096], P('tp'), may hold values from 0.1 to 1.9
Outputs:
- layer_out: bfloat16 [2048, 4096], P(('grp', 'ep'), 'tp'), parts along dimension 0
The draws below stay inside these ranges and needn't reach their ends.
There are 2 independent parts, one for each index of `grp`. The reference program is written for one: setup_inputs(seed, part) draws one part's arguments, and reference() takes and returns one part's arrays. A program takes and returns all parts, laid end to end along the dimension named above; an argument that names none is the same for every part. Nothing has to cross between parts.
Inputs may be any that keep to these rules, and one draw needn't show every extreme that they name: `routes`: each row names 4 different experts; among the rows of one index of ep no expert is named more than 128 times, and in some such block some expert is named exactly 128 times.
All inputs are finite; a program needn't handle non-finite values.
Results may differ from the reference program's by a relative error of at most 0.023.
Values may be sent and summed in bfloat16 or wider, within the bound.
A program may use at most 64 MiB of HBM per device.

```python
import math
import jax
import jax.numpy as jnp
import numpy as np
from jax import lax

D = 4096
FF = 1024
FS = 1024
TOP_K = 4
TOK_EP = 128
EXPERTS = 8
CAP = 128
TOKENS = 1024
N_TP = 2


def rising_columns(key, width):
    base = jnp.exp(jnp.linspace(0.0, math.log(4.0), width, dtype=jnp.float32))
    jitter = jax.random.uniform(key, (width,), jnp.float32, 0.8, 1.2)
    return base * jitter


def draw_expert_down(key, part):
    noise = jax.random.normal(jax.random.fold_in(key, 11), (EXPERTS, FF, D), jnp.float32)
    rise = rising_columns(jax.random.fold_in(key, 12), D)
    return (noise * rise * FF ** (-0.5)).astype(jnp.bfloat16)


def draw_shared_down(key, part):
    noise = jax.random.normal(jax.random.fold_in(key, 21), (FS, D), jnp.float32)
    rise = rising_columns(jax.random.fold_in(key, 22), D)
    return (noise * rise * FS ** (-0.5)).astype(jnp.bfloat16)


def level_of(rng, extent, pieces, least, high):
    level = 1.0
    for position, shards_of in pieces:
        steps = jax.random.uniform(jax.random.fold_in(jax.random.fold_in(rng, 6), position), (shards_of,), jnp.float32, least / len(pieces), high / len(pieces))
        level = level * jnp.repeat(jnp.exp(steps), extent[position] // shards_of).reshape((-1,) + (1,) * (len(extent) - 1 - position))
    return level


def shared_out(own_key, own, number, rows, count, top, reach, lean):
    sequence = jax.random.permutation(own_key, count)
    crowded, usual = load_shares(count, rows * top, reach, lean, True), load_shares(count, rows * top, reach, lean, False)
    places = jnp.arange(count)

    def named(sizes, rotation):
        used = int((sizes > 0).sum())
        fixed = max(1, used // 4)
        shifted = fixed + (places - fixed + rotation * (used - fixed)) % max(1, count - fixed)
        return jnp.zeros((count,), jnp.int32).at[sequence[jnp.where(places < fixed, places, shifted)]].set(jnp.asarray(sizes, jnp.int32))

    sizes = jnp.where(number % 4 == 0, named(crowded, number // 4), named(usual, number - number // 4 - 1))
    mixed = jax.random.permutation(jax.random.fold_in(own, 3), count)
    giver, receiver = mixed[0:count // 2 * 2:2], mixed[1:count // 2 * 2:2]
    room = jnp.minimum(sizes[giver] - 1, reach - sizes[receiver]) // 2
    room = jnp.where((giver == sequence[0]) | (receiver == sequence[0]) | (sizes[receiver] == 0), 0, jnp.maximum(room, 0))
    shifted = jax.random.randint(jax.random.fold_in(own, 4), (count // 2,), 0, 1 << 20) % (room + 1)
    sizes = sizes.at[giver].add(-shifted).at[receiver].add(shifted)
    labels = jnp.searchsorted(jnp.cumsum(sizes), jnp.arange(rows * top), side="right").astype(jnp.int32)
    table = labels.reshape(top, rows).T
    table = table[jax.random.permutation(jax.random.fold_in(own, 1), rows)]
    rotation = jax.random.randint(jax.random.fold_in(own, 2), (rows, 1), 0, top)
    return jnp.take_along_axis(table, (jnp.arange(top)[None, :] + rotation) % top, axis=1)


def load_shares(number_of, total, reach, slope, full):
    portions = [(1 << 20) // math.isqrt(rank ** slope) + 1 for rank in range(1, number_of + 1)]
    largest = reach if full else min(reach, max(-(-total // number_of), total * portions[0] // sum(portions)))
    least = 1 if total - largest >= number_of - 1 else 0
    counts, surplus = [largest] + [least] * (number_of - 1), total - largest - least * (number_of - 1)
    while surplus > 0:
        candidates = [i for i in range(1, number_of) if counts[i] < largest] or [i for i in range(1, number_of) if counts[i] < reach]
        pool, remaining = sum([portions[i] for i in candidates]), surplus
        for i in candidates:
            more = min(reach - counts[i], max(1, remaining * portions[i] // pool), surplus)
            counts[i] = counts[i] + more
            surplus = surplus - more
    return np.array(counts)


def normal_values(rng, shape, deviation, reach, split=(), kind=jnp.bfloat16):
    gain = level_of(rng, shape, split, -0.22, 0.18) if split else 1.0
    values = jax.random.normal(rng, shape, jnp.float32) * deviation * gain
    return jnp.minimum(jnp.maximum(values, -reach), reach).astype(kind)


def setup_inputs(seed: int = 0, part: int = 0) -> dict:
    key_of = jax.random.split(jax.random.key(seed), 12)
    part_keys = jax.random.split(jax.random.fold_in(key_of[11], part), 12)
    tokens = normal_values(part_keys[0], (TOKENS, D), 1.0, 6.0, ((0, 8), (1, 2)))
    routes_keys = jax.random.split(jax.random.fold_in(part_keys[1], 1), TOKENS // TOK_EP)
    routes_turns = jax.random.permutation(jax.random.fold_in(part_keys[1], 3), TOKENS // TOK_EP)
    routes = jax.vmap(lambda own, number: shared_out(jax.random.fold_in(part_keys[1], 2), own, number, TOK_EP, EXPERTS, TOP_K, CAP, 2))(routes_keys, routes_turns).reshape((TOKENS, TOP_K))
    route_weights = jnp.clip(jnp.exp(math.log(1.0) - 2.3025851 * jax.random.uniform(part_keys[2], (TOKENS, TOP_K), jnp.float32) ** level_of(part_keys[2], (TOKENS, TOP_K), ((0, 8),), -0.2, 0.2)), 0.1, 1.0)
    norm_gain = jnp.clip(1.0 + 0.18 * jax.random.normal(key_of[3], (D,), jnp.float32), 0.1, 1.9)
    expert_gate = normal_values(key_of[4], (EXPERTS, D, FF), D ** -0.5, 0.09375, ((0, 8), (1, 2)))
    expert_up = normal_values(key_of[5], (EXPERTS, D, FF), D ** -0.5, 0.09375, ((0, 8), (1, 2)))
    expert_down = draw_expert_down(jax.random.fold_in(key_of[11], 71), part)
    shared_gate = normal_values(key_of[7], (D, FS), D ** -0.5, 0.09375, ((0, 2),))
    shared_up = normal_values(key_of[8], (D, FS), D ** -0.5, 0.09375, ((0, 2),))
    shared_down = draw_shared_down(jax.random.fold_in(key_of[11], 71), part)
    out_gain = jnp.clip(1.0 + 0.18 * jax.random.normal(key_of[10], (D,), jnp.float32), 0.1, 1.9)
    return dict(tokens=tokens, routes=routes, route_weights=route_weights, norm_gain=norm_gain, expert_gate=expert_gate, expert_up=expert_up, expert_down=expert_down, shared_gate=shared_gate, shared_up=shared_up, shared_down=shared_down, out_gain=out_gain)


epsilon = 1e-06

def blocked_product(source, matrix):
    rows = source.shape[0]
    source_blocks = source.reshape(rows, N_TP, -1).astype(jnp.float32)
    matrix_blocks = matrix.reshape(N_TP, -1, matrix.shape[1]).astype(jnp.float32)
    partial_value = jnp.einsum('rbf,bfh->brh', source_blocks, matrix_blocks)
    rounded = lax.optimization_barrier(partial_value.astype(jnp.bfloat16))
    return lax.optimization_barrier(jnp.sum(rounded.astype(jnp.float32), axis=0))

def expert_hidden(source, gate_matrix, up_matrix):
    gate_part = blocked_product(source, gate_matrix)
    up_part = blocked_product(source, up_matrix)
    return (jax.nn.silu(gate_part) * up_part).astype(jnp.bfloat16)

def reference(tokens, routes, route_weights, norm_gain, expert_gate, expert_up, expert_down, shared_gate, shared_up, shared_down, out_gain):
    full_float = tokens.astype(jnp.float32)
    normed = (full_float * lax.rsqrt(lax.optimization_barrier(jnp.mean(full_float * full_float, axis=-1, keepdims=True)) + epsilon) * norm_gain).astype(jnp.bfloat16)
    choose = (routes[:, :, None] == jnp.arange(EXPERTS, dtype=jnp.int32)[None, None, :]).astype(jnp.float32)
    weight_table = lax.optimization_barrier(jnp.sum(route_weights[:, :, None] * choose, axis=1))

    def add_expert(totals, expert):
        hidden = expert_hidden(normed, expert_gate[expert], expert_up[expert])
        expert_rows = jnp.dot(hidden, expert_down[expert], preferred_element_type=jnp.float32).astype(jnp.bfloat16)
        column = lax.dynamic_slice_in_dim(weight_table, expert, 1, 1)
        return (totals + column * expert_rows.astype(jnp.float32), None)
    routed, _ = lax.scan(add_expert, jnp.zeros((normed.shape[0], D), jnp.float32), jnp.arange(EXPERTS, dtype=jnp.int32))
    shared_hidden = expert_hidden(normed, shared_gate, shared_up)
    mixture = routed + jnp.dot(shared_hidden, shared_down, preferred_element_type=jnp.float32)
    scale = lax.rsqrt(lax.optimization_barrier(jnp.mean(mixture * mixture, axis=-1, keepdims=True)) + epsilon)
    return (mixture * scale * out_gain).astype(jnp.bfloat16)
```

```python
import functools

import jax
import jax.numpy as jnp
from jax import lax
from jax.experimental import pallas as pl
from jax.experimental.pallas import tpu as pltpu
from jax.sharding import PartitionSpec as P

epsilon = 1e-06
MESH = pl.DeviceIdType.MESH
TABLE = 128


def plan(chips):
    steps = [(0, 0), None, (1, 0)]
    for mask in range(2, chips):
        steps += [(mask, 0), (mask, 1)]
    steps += [(1, 1), (0, 1)]
    relays = []
    for distance in range(1, chips):
        relays.append(next(i for i, s in enumerate(steps) if s is not None and s[0] >= distance))
    return steps, relays


def pick(index, table):
    value = jnp.int32(table[0])
    for position in range(1, len(table)):
        if table[position] != table[0]:
            value = jnp.where(index == position, jnp.int32(table[position]), value)
    return value


def exclusive_or(a, b, size):
    total, unit = jnp.int32(0), 1
    while unit < size:
        total = total + unit * lax.rem(lax.div(a, unit) + lax.div(b, unit), 2)
        unit *= 2
    return total


def fused_kernel(
    chips,
    tokens_ref,
    routes_ref,
    weights_ref,
    norm_gain_ref,
    gate_hbm,
    up_hbm,
    down_hbm,
    shared_gate_hbm,
    shared_up_hbm,
    shared_down_hbm,
    out_gain_ref,
    out_ref,
    gate,
    up,
    down,
    held,
    part_out,
    part_in,
    part_own,
    hidden,
    product,
    pair_out,
    pair_in,
    far_out,
    far_in,
    mixture,
    square_out,
    square_in,
    load_sem,
    square_send,
    square_recv,
    gather_send,
    gather_recv,
    pair_gather_recv,
    part_send,
    part_recv,
    hidden_send,
    hidden_recv,
    pair_send,
    pair_recv,
    far_send,
    far_recv,
):
    rows, width = tokens_ref.shape
    experts = 2 * chips
    units = gate.shape[2]
    half = units // 2
    steps, relays = plan(chips)
    count = len(steps)
    masks = [0 if s is None else s[0] for s in steps]
    lanes = [0 if s is None else s[1] for s in steps]
    shared_at = steps.index(None)

    ep = lax.axis_index("ep")
    tp = lax.axis_index("tp")
    chip, core = lax.div(ep, 2), lax.rem(ep, 2)
    other_core = 1 - core
    partner = {"ep": chip * 2 + other_core}
    across = {"tp": 1 - tp}

    loads = [
        pltpu.make_async_copy(source, target, load_sem.at[i])
        for i, (source, target) in enumerate(
            [
                (gate_hbm.at[0], gate.at[0]),
                (up_hbm.at[0], up.at[0]),
                (shared_gate_hbm, gate.at[1]),
                (shared_up_hbm, up.at[1]),
                (down_hbm.at[0], down.at[0]),
                (shared_down_hbm, down.at[1]),
            ]
        )
    ]
    for load in loads:
        load.start()

    barrier = pltpu.get_barrier_semaphore()
    for shift in range(1, chips):
        pl.semaphore_signal(
            barrier,
            inc=1,
            device_id={"ep": lax.rem(chip + shift, chips) * 2 + core},
            device_id_type=MESH,
        )
    pl.semaphore_signal(barrier, inc=1, device_id=partner, device_id_type=MESH)
    pl.semaphore_signal(barrier, inc=1, device_id=across, device_id_type=MESH)

    def remote(source, target, send, recv, device):
        return pltpu.make_async_remote_copy(
            src_ref=source,
            dst_ref=target,
            send_sem=send,
            recv_sem=recv,
            device_id=device,
            device_id_type=MESH,
        )

    def square_copy(which):
        return remote(
            square_out.at[which],
            square_in.at[which],
            square_send.at[which],
            square_recv.at[which],
            across,
        )

    def gather_copy(origin, way):
        slot = held.at[origin * 2 + core]
        device = ({"ep": (chip - 1) * 2 + core}, {"ep": (chip + 1) * 2 + core}, partner)[way]
        recv = (pair_gather_recv if way == 2 else gather_recv).at[origin]
        return remote(slot, slot, gather_send.at[origin, way], recv, device)

    def pair_gather_arrival(origin):
        slot = held.at[origin * 2 + other_core]
        return remote(slot, slot, gather_send.at[origin, 2], pair_gather_recv.at[origin], partner)

    def part_copy(k):
        return remote(part_out.at[k], part_in.at[k], part_send.at[k], part_recv.at[k], across)

    def hidden_copy(k, side):
        return remote(
            hidden.at[k, side], hidden.at[k, side], hidden_send.at[k], hidden_recv.at[k], across
        )

    def pair_copy(origin):
        return remote(
            pair_out.at[origin],
            pair_in.at[origin],
            pair_send.at[origin],
            pair_recv.at[origin],
            partner,
        )

    def far_copy(target):
        return remote(
            far_out.at[target],
            far_in.at[chip],
            far_send.at[target],
            far_recv.at[chip],
            {"ep": target * 2 + core},
        )

    def far_arrival(source):
        return remote(
            far_out.at[source],
            far_in.at[source],
            far_send.at[source],
            far_recv.at[source],
            {"ep": source * 2 + core},
        )

    token_float = tokens_ref[...].astype(jnp.float32)
    square_out[0] = jnp.broadcast_to(
        jnp.sum(token_float * token_float, axis=-1, keepdims=True), (rows, 128)
    )
    pl.semaphore_wait(barrier, chips + 1)
    square_copy(0).start()
    lane_ids = lax.broadcasted_iota(jnp.int32, (rows, TABLE), 1)
    table = jnp.zeros((rows, TABLE), jnp.float32)
    for choice in range(routes_ref.shape[1]):
        named = routes_ref[:, choice : choice + 1]
        match = (lane_ids == named) | (lane_ids == named + experts)
        table = table + jnp.where(match, weights_ref[:, choice : choice + 1], 0.0)
    coarse = table.astype(jnp.bfloat16).astype(jnp.float32)
    held[ep, :, width:] = jnp.where(lane_ids < experts, table, table - coarse).astype(jnp.bfloat16)
    mixture[...] = jnp.zeros_like(mixture)
    square_copy(0).wait_recv()
    square = (square_out[0] + square_in[0])[:, :1]
    gain = norm_gain_ref[:, pl.ds(pl.multiple_of(tp * width, width), width)]
    held[ep, :, :width] = (
        tokens_ref[...].astype(jnp.float32) * lax.rsqrt(square / (2 * width) + epsilon) * gain
    ).astype(jnp.bfloat16)

    gather_copy(chip, 2).start()

    @pl.when(chip > 0)
    def _():
        gather_copy(chip, 0).start()

    @pl.when(chip < chips - 1)
    def _():
        gather_copy(chip, 1).start()

    def locate(k):
        origin = exclusive_or(chip, pick(k, masks), chips)
        lane = pick(k, lanes)
        return origin, lane

    def first_stage(k):
        origin, lane = locate(k)
        is_shared = k == shared_at

        @pl.when(k == 0)
        def _():
            loads[0].wait()
            loads[1].wait()

        @pl.when(is_shared)
        def _():
            loads[2].wait()
            loads[3].wait()

        for index, position in enumerate(relays):
            distance = index + 1

            @pl.when((k == position) & (chip >= distance))
            def _(distance=distance):
                gather_copy(chip - distance, 0).wait_recv()
                gather_copy(chip - distance, 2).start()

                @pl.when(chip < chips - 1)
                def _():
                    gather_copy(chip - distance, 1).start()

            @pl.when((k == position) & (chip + distance < chips))
            def _(distance=distance):
                gather_copy(chip + distance, 1).wait_recv()
                gather_copy(chip + distance, 2).start()

                @pl.when(chip > 0)
                def _():
                    gather_copy(chip + distance, 0).start()

        @pl.when((lane != core) & (k != shared_at))
        def _():
            pair_gather_arrival(origin).wait_recv()

        block = jnp.where(is_shared, ep, origin * 2 + lane)
        kind = jnp.where(is_shared, 1, 0)
        source = held[block, :, :width]
        away = pl.ds(pl.multiple_of((1 - tp) * half, half), half)
        near = pl.ds(pl.multiple_of(tp * half, half), half)
        for which, matrix in enumerate((gate, up)):
            part_out[k, which] = jnp.dot(
                source, matrix[kind, :, away], preferred_element_type=jnp.float32
            ).astype(jnp.bfloat16)
        part_copy(k).start()
        for which, matrix in enumerate((gate, up)):
            part_own[k, which] = jnp.dot(
                source, matrix[kind, :, near], preferred_element_type=jnp.float32
            ).astype(jnp.bfloat16)

    def second_stage(k):
        part_copy(k).wait_recv()
        gate_sum = part_own[k, 0].astype(jnp.float32) + part_in[k, 0].astype(jnp.float32)
        up_sum = part_own[k, 1].astype(jnp.float32) + part_in[k, 1].astype(jnp.float32)
        hidden[k, tp] = (jax.nn.silu(gate_sum) * up_sum).astype(jnp.bfloat16)
        hidden_copy(k, tp).start()

    def third_stage(k):
        origin, lane = locate(k)
        is_shared = k == shared_at

        @pl.when(k == 0)
        def _():
            loads[4].wait()
            loads[5].wait()

        hidden_copy(k, 1 - tp).wait_recv()
        block = jnp.where(is_shared, ep, origin * 2 + lane)
        kind = jnp.where(is_shared, 1, 0)
        chosen = (lane_ids == ep) | (lane_ids == ep + experts)
        scale = jnp.sum(
            jnp.where(chosen, held[block, :, width:].astype(jnp.float32), 0.0),
            axis=-1,
            keepdims=True,
        )
        tile = width // 4

        def tile_step(i, carry):
            columns = pl.ds(pl.multiple_of(i * tile, tile), tile)
            product[:, columns] = jnp.dot(
                hidden[k, 0], down[kind, :half, columns], preferred_element_type=jnp.float32
            ) + jnp.dot(
                hidden[k, 1], down[kind, half:, columns], preferred_element_type=jnp.float32
            )
            return carry

        lax.fori_loop(0, 4, tile_step, 0)

        def weighted():
            return product[...].astype(jnp.bfloat16).astype(jnp.float32) * scale

        @pl.when(is_shared)
        def _():
            mixture[...] += product[...]

        @pl.when((k != shared_at) & (lane != core))
        def _():
            pair_out[origin] = weighted().astype(jnp.bfloat16)
            pair_copy(origin).start()

        @pl.when((k != shared_at) & (lane == core))
        def _():
            pair_copy(origin).wait_recv()

            @pl.when(origin == chip)
            def _():
                mixture[...] += weighted() + pair_in[origin].astype(jnp.float32)

            @pl.when(origin != chip)
            def _():
                far_out[origin] = (weighted() + pair_in[origin].astype(jnp.float32)).astype(
                    jnp.bfloat16
                )
                far_copy(origin).start()

    def body(i, carry):
        @pl.when(i < count)
        def _():
            first_stage(i)

        @pl.when((i >= 1) & (i < count + 1))
        def _():
            second_stage(i - 1)

        @pl.when(i >= 2)
        def _():
            third_stage(i - 2)

        return carry

    lax.fori_loop(0, count + 2, body, 0)

    for shift in range(1, chips):
        source = lax.rem(chip + shift, chips)
        far_arrival(source).wait_recv()
        mixture[...] += far_in[source].astype(jnp.float32)

    mixed = mixture[...]
    square_out[1] = jnp.broadcast_to(jnp.sum(mixed * mixed, axis=-1, keepdims=True), (rows, 128))
    square_copy(1).start()
    square_copy(1).wait_recv()
    total = (square_out[1] + square_in[1])[:, :1]
    out_ref[...] = (
        mixture[...] * lax.rsqrt(total / (2 * width) + epsilon) * out_gain_ref[...]
    ).astype(jnp.bfloat16)

    square_copy(0).wait_send()
    square_copy(1).wait_send()
    for origin in range(chips):
        gather_copy(origin, 2).wait_send()
        pair_copy(origin).wait_send()

        @pl.when((chip >= origin) & (chip < chips - 1))
        def _(origin=origin):
            gather_copy(origin, 1).wait_send()

        @pl.when((chip <= origin) & (chip > 0))
        def _(origin=origin):
            gather_copy(origin, 0).wait_send()

        @pl.when(chip != origin)
        def _(origin=origin):
            far_copy(origin).wait_send()

    def drain(k, carry):
        part_copy(k).wait_send()
        hidden_copy(k, tp).wait_send()
        return carry

    lax.fori_loop(0, count, drain, 0)


def fused(
    chips,
    tokens,
    routes,
    route_weights,
    norm_gain,
    expert_gate,
    expert_up,
    expert_down,
    shared_gate,
    shared_up,
    shared_down,
    out_gain,
):
    rows, width = tokens.shape
    units = shared_gate.shape[1]
    half = units // 2
    count = 2 * chips + 1
    vmem = pl.BlockSpec(memory_space=pltpu.VMEM)
    hbm = pl.BlockSpec(memory_space=pl.ANY)
    bf16, f32 = jnp.bfloat16, jnp.float32
    dma = pltpu.SemaphoreType.DMA
    return pl.pallas_call(
        functools.partial(fused_kernel, chips),
        out_shape=jax.ShapeDtypeStruct((rows, width), bf16),
        in_specs=[vmem] * 4 + [hbm] * 6 + [vmem],
        out_specs=vmem,
        scratch_shapes=[
            pltpu.VMEM((2, width, units), bf16),
            pltpu.VMEM((2, width, units), bf16),
            pltpu.VMEM((2, units, width), bf16),
            pltpu.VMEM((2 * chips, rows, width + TABLE), bf16),
            pltpu.VMEM((count, 2, rows, half), bf16),
            pltpu.VMEM((count, 2, rows, half), bf16),
            pltpu.VMEM((count, 2, rows, half), bf16),
            pltpu.VMEM((count, 2, rows, half), bf16),
            pltpu.VMEM((rows, width), f32),
            pltpu.VMEM((chips, rows, width), bf16),
            pltpu.VMEM((chips, rows, width), bf16),
            pltpu.VMEM((chips, rows, width), bf16),
            pltpu.VMEM((chips, rows, width), bf16),
            pltpu.VMEM((rows, width), f32),
            pltpu.VMEM((2, rows, 128), f32),
            pltpu.VMEM((2, rows, 128), f32),
            dma((6,)),
            dma((2,)),
            dma((2,)),
            dma((chips, 3)),
            dma((chips,)),
            dma((chips,)),
            dma((count,)),
            dma((count,)),
            dma((count,)),
            dma((count,)),
            dma((chips,)),
            dma((chips,)),
            dma((chips,)),
            dma((chips,)),
        ],
        compiler_params=pltpu.CompilerParams(
            collective_id=0, has_side_effects=True, vmem_limit_bytes=60 * 1024 * 1024
        ),
    )(
        tokens,
        routes,
        route_weights,
        norm_gain.reshape(1, -1),
        expert_gate,
        expert_up,
        expert_down,
        shared_gate,
        shared_up,
        shared_down,
        out_gain.reshape(1, -1),
    )


def local_product(source, matrix):
    return jnp.dot(source, matrix, preferred_element_type=jnp.float32)


def per_device(
    tokens,
    routes,
    route_weights,
    norm_gain,
    expert_gate,
    expert_up,
    expert_down,
    shared_gate,
    shared_up,
    shared_down,
    out_gain,
):
    block_width = tokens.shape[1]
    full_width = block_width * lax.axis_size("tp")
    width_index = lax.axis_index("tp")
    full_rows = lax.all_gather(tokens, "tp", axis=1, tiled=True)
    full_float = full_rows.astype(jnp.float32)
    normed_full = (
        full_float
        * lax.rsqrt(jnp.mean(full_float * full_float, axis=-1, keepdims=True) + epsilon)
        * norm_gain
    ).astype(jnp.bfloat16)
    normed_block = lax.dynamic_slice_in_dim(normed_full, width_index * block_width, block_width, 1)
    gate_matrix = expert_gate[0]
    up_matrix = expert_up[0]
    down_matrix = expert_down[0]
    experts = lax.axis_size("ep")
    choose = (routes[:, :, None] == jnp.arange(experts, dtype=jnp.int32)[None, None, :]).astype(
        jnp.float32
    )
    weight_table = jnp.sum(route_weights[:, :, None] * choose, axis=1)
    expert_input = lax.all_gather(normed_block, "ep", axis=0, tiled=True)
    table_all = lax.all_gather(weight_table, "ep", axis=0, tiled=True)
    summed = (
        lax.psum(local_product(expert_input, gate_matrix).astype(jnp.bfloat16), "tp").astype(
            jnp.float32
        ),
        lax.psum(local_product(expert_input, up_matrix).astype(jnp.bfloat16), "tp").astype(
            jnp.float32
        ),
        lax.psum(local_product(normed_block, shared_gate).astype(jnp.bfloat16), "tp").astype(
            jnp.float32
        ),
        lax.psum(local_product(normed_block, shared_up).astype(jnp.bfloat16), "tp").astype(
            jnp.float32
        ),
    )
    routed_hidden = (jax.nn.silu(summed[0]) * summed[1]).astype(jnp.bfloat16)
    shared_hidden = (jax.nn.silu(summed[2]) * summed[3]).astype(jnp.bfloat16)
    expert_rows = local_product(routed_hidden, down_matrix).astype(jnp.bfloat16)
    shared_out = local_product(shared_hidden, shared_down)
    own_expert = lax.axis_index("ep")
    column = lax.dynamic_slice_in_dim(table_all, own_expert, 1, 1)
    routed = lax.psum_scatter(
        (column * expert_rows.astype(jnp.float32)).astype(jnp.bfloat16),
        "ep",
        scatter_dimension=0,
        tiled=True,
    ).astype(jnp.float32)
    mixture = routed + shared_out
    square_sum = lax.psum(jnp.sum(mixture * mixture, axis=-1, keepdims=True), "tp")
    scale = lax.rsqrt(square_sum / full_width + epsilon)
    return (mixture * scale * out_gain).astype(jnp.bfloat16)


def solution(mesh):
    chips = mesh.shape["ep"] // 2
    powers = chips >= 2 and chips & (chips - 1) == 0 and mesh.shape["ep"] % 2 == 0
    if mesh.shape["tp"] == 2 and powers and chips * 4 <= TABLE:
        body = functools.partial(fused, chips)
    else:
        body = per_device
    return jax.shard_map(
        body,
        mesh=mesh,
        in_specs=(
            P(("grp", "ep"), "tp"),
            P(("grp", "ep"), None),
            P(("grp", "ep"), None),
            P(),
            P("ep", "tp", None),
            P("ep", "tp", None),
            P("ep", None, "tp"),
            P("tp", None),
            P("tp", None),
            P(None, "tp"),
            P("tp"),
        ),
        out_specs=P(("grp", "ep"), "tp"),
        check_vma=False,
    )
```

```python
import functools

import jax
import jax.numpy as jnp
from jax import lax
from jax.experimental import pallas as pl
from jax.experimental.pallas import tpu as pltpu
from jax.sharding import PartitionSpec as P

epsilon = 1e-06
MESH = pl.DeviceIdType.MESH
TABLE = 128


def plan(chips):
    ring = [mask for mask in range(2, chips)]
    first = [(0, 0), (0, 1), (1, 0)]
    steps = first + [(mask, 0) for mask in ring] + [(mask, 1) for mask in ring] + [(1, 1), None]
    relays = [[steps.index((distance, 0)), steps.index((max(distance, 2), 1))] for distance in range(1, chips)]
    relays[0][1] -= 1
    return steps, relays


def pick(index, table):
    value = jnp.int32(table[0])
    for position in range(1, len(table)):
        if table[position] != table[0]:
            value = jnp.where(index == position, jnp.int32(table[position]), value)
    return value


def exclusive_or(a, b, size):
    total, unit = jnp.int32(0), 1
    while unit < size:
        total = total + unit * lax.rem(lax.div(a, unit) + lax.div(b, unit), 2)
        unit *= 2
    return total


def fused_kernel(
    chips,
    tokens_hbm,
    routes_hbm,
    weights_hbm,
    norm_gain_hbm,
    gate_hbm,
    up_hbm,
    down_hbm,
    shared_gate_hbm,
    shared_up_hbm,
    shared_down_hbm,
    out_gain_hbm,
    out_ref,
    tokens_ref,
    routes_ref,
    weights_ref,
    norm_gain_ref,
    out_gain_ref,
    gate,
    up,
    down,
    held,
    part_out,
    part_in,
    part_own,
    hidden,
    product,
    waiting,
    pair_out,
    pair_in,
    far_out,
    far_in,
    mixture,
    square_out,
    square_in,
    load_sem,
    square_send,
    square_recv,
    gather_send,
    gather_recv,
    pair_gather_recv,
    part_send,
    part_recv,
    hidden_send,
    hidden_recv,
    pair_send,
    pair_recv,
    far_send,
    far_recv,
):
    rows, width = tokens_ref.shape
    experts = 2 * chips
    units = gate.shape[2]
    half = units // 2
    steps, relays = plan(chips)
    count = len(steps)
    masks = [0 if s is None else s[0] for s in steps]
    lanes = [0 if s is None else s[1] for s in steps]
    shared_at = steps.index(None)

    ep = lax.axis_index("ep")
    tp = lax.axis_index("tp")
    chip, core = lax.div(ep, 2), lax.rem(ep, 2)
    other_core = 1 - core
    partner = {"ep": chip * 2 + other_core}
    across = {"tp": 1 - tp}

    loads = [
        pltpu.make_async_copy(source, target, load_sem.at[i])
        for i, (source, target) in enumerate(
            [
                (gate_hbm.at[0], gate.at[0]),
                (up_hbm.at[0], up.at[0]),
                (shared_gate_hbm, gate.at[1]),
                (shared_up_hbm, up.at[1]),
                (down_hbm.at[0], down.at[0]),
                (shared_down_hbm, down.at[1]),
                (tokens_hbm, tokens_ref),
                (routes_hbm, routes_ref),
                (weights_hbm, weights_ref),
                (norm_gain_hbm, norm_gain_ref),
                (out_gain_hbm, out_gain_ref),
            ]
        )
    ]
    for load in loads[6:] + loads[:2]:
        load.start()

    barrier = pltpu.get_barrier_semaphore()
    for shift in range(1, chips):
        pl.semaphore_signal(
            barrier,
            inc=1,
            device_id={"ep": lax.rem(chip + shift, chips) * 2 + core},
            device_id_type=MESH,
        )
    pl.semaphore_signal(barrier, inc=1, device_id=partner, device_id_type=MESH)
    pl.semaphore_signal(barrier, inc=1, device_id=across, device_id_type=MESH)

    def remote(source, target, send, recv, device):
        return pltpu.make_async_remote_copy(
            src_ref=source,
            dst_ref=target,
            send_sem=send,
            recv_sem=recv,
            device_id=device,
            device_id_type=MESH,
        )

    def square_copy(which):
        return remote(
            square_out.at[which],
            square_in.at[which],
            square_send.at[which],
            square_recv.at[which],
            across,
        )

    def gather_copy(origin, way):
        slot = held.at[origin * 2 + core]
        device = ({"ep": (chip - 1) * 2 + core}, {"ep": (chip + 1) * 2 + core}, partner)[way]
        recv = (pair_gather_recv if way == 2 else gather_recv).at[origin]
        return remote(slot, slot, gather_send.at[origin, way], recv, device)

    def pair_gather_arrival(origin):
        slot = held.at[origin * 2 + other_core]
        return remote(slot, slot, gather_send.at[origin, 2], pair_gather_recv.at[origin], partner)

    def part_copy(k):
        return remote(part_out.at[k], part_in.at[k], part_send.at[k], part_recv.at[k], across)

    def hidden_copy(k, side):
        return remote(
            hidden.at[k, side], hidden.at[k, side], hidden_send.at[k], hidden_recv.at[k], across
        )

    def pair_copy(origin):
        return remote(
            pair_out.at[origin],
            pair_in.at[origin],
            pair_send.at[origin],
            pair_recv.at[origin],
            partner,
        )

    beside, opposite, beyond = (exclusive_or(chip, mask, chips) for mask in (1, 2, 3))

    def far_copy(mask, origin):
        slot = jnp.where(mask == 2, beyond, chip)
        return remote(
            far_out.at[origin],
            far_in.at[slot],
            far_send.at[origin],
            far_recv.at[slot],
            {"ep": jnp.where(mask == 3, beyond, beside) * 2 + core},
        )

    def far_arrival(slot):
        return remote(
            far_out.at[slot],
            far_in.at[slot],
            far_send.at[slot],
            far_recv.at[slot],
            {"ep": beside * 2 + core},
        )

    def pack(column):
        return jnp.transpose(jnp.broadcast_to(column, (rows, 128)))[:8]

    def unpack(row):
        return jnp.transpose(jnp.broadcast_to(row[:1], (128, rows)))[:, :1]

    for load in loads[6:]:
        load.wait()
    token_float = tokens_ref[...].astype(jnp.float32)
    own_square = jnp.sum(token_float * token_float, axis=-1, keepdims=True)
    square_out[0] = pack(own_square)
    pl.semaphore_wait(barrier, chips + 1)
    square_copy(0).start()
    lane_ids = lax.broadcasted_iota(jnp.int32, (rows, TABLE), 1)
    expert_ids = lax.broadcasted_iota(jnp.int32, (TABLE, rows), 0)
    table = jnp.zeros((TABLE, rows), jnp.float32)
    for choice in range(routes_ref.shape[0]):
        named = routes_ref[choice : choice + 1, :]
        match = (expert_ids == named) | (expert_ids == named + experts)
        table = table + jnp.where(match, weights_ref[choice : choice + 1, :], 0.0)
    table = jnp.transpose(table)
    coarse = table.astype(jnp.bfloat16).astype(jnp.float32)
    held[ep, :, width:] = jnp.where(lane_ids < experts, table, table - coarse).astype(jnp.bfloat16)
    mixture[...] = jnp.zeros_like(mixture)
    square_copy(0).wait_recv()
    square = own_square + unpack(square_in[0])
    gain = norm_gain_ref[:, pl.ds(pl.multiple_of(tp * width, width), width)]
    held[ep, :, :width] = (
        tokens_ref[...].astype(jnp.float32) * lax.rsqrt(square / (2 * width) + epsilon) * gain
    ).astype(jnp.bfloat16)

    def send_outward():
        @pl.when(chip > 0)
        def _():
            gather_copy(chip, 0).start()

        @pl.when(chip < chips - 1)
        def _():
            gather_copy(chip, 1).start()

    gather_copy(chip, 2).start()
    pl.when(core == 0)(send_outward)

    def locate(k):
        origin = exclusive_or(chip, pick(k, masks), chips)
        lane = pick(k, lanes)
        return origin, lane

    def first_stage(k):
        origin, lane = locate(k)
        is_shared = k == shared_at

        @pl.when(k == 0)
        def _():
            loads[0].wait()
            loads[1].wait()
            for load in loads[2:6]:
                load.start()

        @pl.when(is_shared)
        def _():
            loads[2].wait()
            loads[3].wait()

        for index, positions in enumerate(relays):
            distance = index + 1
            position = jnp.where(core == 0, positions[0], positions[1])

            @pl.when((k == position) & (chip >= distance))
            def _(distance=distance):
                gather_copy(chip - distance, 0).wait_recv()
                gather_copy(chip - distance, 2).start()

                @pl.when(chip < chips - 1)
                def _():
                    gather_copy(chip - distance, 1).start()

            @pl.when((k == position) & (chip + distance < chips))
            def _(distance=distance):
                gather_copy(chip + distance, 1).wait_recv()
                gather_copy(chip + distance, 2).start()

                @pl.when(chip > 0)
                def _():
                    gather_copy(chip + distance, 0).start()

        @pl.when((lane != core) & (k != shared_at))
        def _():
            pair_gather_arrival(origin).wait_recv()

        block = jnp.where(is_shared, ep, origin * 2 + lane)
        kind = jnp.where(is_shared, 1, 0)
        source = held[block, :, :width]
        away = pl.ds(pl.multiple_of((1 - tp) * half, half), half)
        near = pl.ds(pl.multiple_of(tp * half, half), half)
        for which, matrix in enumerate((gate, up)):
            part_out[k, which] = jnp.dot(
                source, matrix[kind, :, away], preferred_element_type=jnp.float32
            ).astype(jnp.bfloat16)
        part_copy(k).start()
        for which, matrix in enumerate((gate, up)):
            part_own[k, which] = jnp.dot(
                source, matrix[kind, :, near], preferred_element_type=jnp.float32
            ).astype(jnp.bfloat16)

    def second_stage(k):
        part_copy(k).wait_recv()
        gate_sum = part_own[k, 0].astype(jnp.float32) + part_in[k, 0].astype(jnp.float32)
        up_sum = part_own[k, 1].astype(jnp.float32) + part_in[k, 1].astype(jnp.float32)
        hidden[k, tp] = (jax.nn.silu(gate_sum) * up_sum).astype(jnp.bfloat16)
        hidden_copy(k, tp).start()

    def third_stage(k):
        origin, lane = locate(k)
        is_shared = k == shared_at

        @pl.when(k == 0)
        def _():
            loads[4].wait()
            loads[5].wait()

        hidden_copy(k, 1 - tp).wait_recv()
        block = jnp.where(is_shared, ep, origin * 2 + lane)
        kind = jnp.where(is_shared, 1, 0)
        chosen = (lane_ids == ep) | (lane_ids == ep + experts)
        scale = jnp.sum(
            jnp.where(chosen, held[block, :, width:].astype(jnp.float32), 0.0),
            axis=-1,
            keepdims=True,
        )
        tile = width // 4

        def tile_step(i, carry):
            columns = pl.ds(pl.multiple_of(i * tile, tile), tile)
            product[:, columns] = jnp.dot(
                hidden[k, 0], down[kind, :half, columns], preferred_element_type=jnp.float32
            ) + jnp.dot(
                hidden[k, 1], down[kind, half:, columns], preferred_element_type=jnp.float32
            )
            return carry

        lax.fori_loop(0, 4, tile_step, 0)

        def weighted():
            return product[...].astype(jnp.bfloat16).astype(jnp.float32) * scale

        @pl.when(is_shared)
        def _():
            mixture[...] += product[...]

        @pl.when((k != shared_at) & (lane != core))
        def _():
            pair_out[origin] = weighted().astype(jnp.bfloat16)
            pair_copy(origin).start()

        @pl.when((k != shared_at) & (lane == core))
        def _():
            waiting[...] = weighted()

    def fourth_stage(k):
        origin, lane = locate(k)

        @pl.when((k != shared_at) & (lane == core))
        def _():
            pair_copy(origin).wait_recv()

            @pl.when(origin == chip)
            def _():
                mixture[...] += waiting[...] + pair_in[origin].astype(jnp.float32)

            mask = pick(k, masks)

            @pl.when(mask == 3)
            def _():
                far_arrival(opposite).wait_recv()
                waiting[...] += far_in[opposite].astype(jnp.float32)

            @pl.when(origin != chip)
            def _():
                far_out[origin] = (waiting[...] + pair_in[origin].astype(jnp.float32)).astype(
                    jnp.bfloat16
                )
                far_copy(mask, origin).start()

    def body(i, carry):
        @pl.when(i < count)
        def _():
            first_stage(i)

        @pl.when(i >= 3)
        def _():
            fourth_stage(i - 3)

        @pl.when((i >= 1) & (i < count + 1))
        def _():
            second_stage(i - 1)

        @pl.when((i == 2) & (core == 1))
        def _():
            send_outward()

        @pl.when((i >= 2) & (i < count + 2))
        def _():
            third_stage(i - 2)

        return carry

    lax.fori_loop(0, count + 3, body, 0)

    far_arrival(beside).wait_recv()
    far_arrival(beyond).wait_recv()
    mixture[...] += far_in[beside].astype(jnp.float32) + far_in[beyond].astype(jnp.float32)

    mixed = mixture[...]
    own_total = jnp.sum(mixed * mixed, axis=-1, keepdims=True)
    square_out[1] = pack(own_total)
    square_copy(1).start()
    square_copy(1).wait_recv()
    total = own_total + unpack(square_in[1])
    out_ref[...] = (
        mixture[...] * lax.rsqrt(total / (2 * width) + epsilon) * out_gain_ref[...]
    ).astype(jnp.bfloat16)

    square_copy(0).wait_send()
    square_copy(1).wait_send()
    for origin in range(chips):
        gather_copy(origin, 2).wait_send()
        pair_copy(origin).wait_send()

        @pl.when((chip >= origin) & (chip < chips - 1))
        def _(origin=origin):
            gather_copy(origin, 1).wait_send()

        @pl.when((chip <= origin) & (chip > 0))
        def _(origin=origin):
            gather_copy(origin, 0).wait_send()

        @pl.when(chip != origin)
        def _(origin=origin):
            far_arrival(origin).wait_send()

    def drain(k, carry):
        part_copy(k).wait_send()
        hidden_copy(k, tp).wait_send()
        return carry

    lax.fori_loop(0, count, drain, 0)


def fused(
    chips,
    tokens,
    routes,
    route_weights,
    norm_gain,
    expert_gate,
    expert_up,
    expert_down,
    shared_gate,
    shared_up,
    shared_down,
    out_gain,
):
    rows, width = tokens.shape
    units = shared_gate.shape[1]
    half = units // 2
    count = 2 * chips + 1
    choices = routes.shape[1]
    vmem = pl.BlockSpec(memory_space=pltpu.VMEM)
    hbm = pl.BlockSpec(memory_space=pl.ANY)
    bf16, f32 = jnp.bfloat16, jnp.float32
    dma = pltpu.SemaphoreType.DMA
    return pl.pallas_call(
        functools.partial(fused_kernel, chips),
        out_shape=jax.ShapeDtypeStruct((rows, width), bf16),
        in_specs=[hbm] * 11,
        out_specs=vmem,
        scratch_shapes=[
            pltpu.VMEM((rows, width), bf16),
            pltpu.VMEM((choices, rows), jnp.int32),
            pltpu.VMEM((choices, rows), f32),
            pltpu.VMEM((1, norm_gain.shape[0]), f32),
            pltpu.VMEM((1, width), f32),
            pltpu.VMEM((2, width, units), bf16),
            pltpu.VMEM((2, width, units), bf16),
            pltpu.VMEM((2, units, width), bf16),
            pltpu.VMEM((2 * chips, rows, width + TABLE), bf16),
            pltpu.VMEM((count, 2, rows, half), bf16),
            pltpu.VMEM((count, 2, rows, half), bf16),
            pltpu.VMEM((count, 2, rows, half), bf16),
            pltpu.VMEM((count, 2, rows, half), bf16),
            pltpu.VMEM((rows, width), f32),
            pltpu.VMEM((rows, width), f32),
            pltpu.VMEM((chips, rows, width), bf16),
            pltpu.VMEM((chips, rows, width), bf16),
            pltpu.VMEM((chips, rows, width), bf16),
            pltpu.VMEM((chips, rows, width), bf16),
            pltpu.VMEM((rows, width), f32),
            pltpu.VMEM((2, 8, rows), f32),
            pltpu.VMEM((2, 8, rows), f32),
            dma((11,)),
            dma((2,)),
            dma((2,)),
            dma((chips, 3)),
            dma((chips,)),
            dma((chips,)),
            dma((count,)),
            dma((count,)),
            dma((count,)),
            dma((count,)),
            dma((chips,)),
            dma((chips,)),
            dma((chips,)),
            dma((chips,)),
        ],
        compiler_params=pltpu.CompilerParams(
            collective_id=0, has_side_effects=True, vmem_limit_bytes=60 * 1024 * 1024
        ),
    )(
        tokens,
        routes.T,
        route_weights.T,
        norm_gain.reshape(1, -1),
        expert_gate,
        expert_up,
        expert_down,
        shared_gate,
        shared_up,
        shared_down,
        out_gain.reshape(1, -1),
    )


def local_product(source, matrix):
    return jnp.dot(source, matrix, preferred_element_type=jnp.float32)


def per_device(
    tokens,
    routes,
    route_weights,
    norm_gain,
    expert_gate,
    expert_up,
    expert_down,
    shared_gate,
    shared_up,
    shared_down,
    out_gain,
):
    block_width = tokens.shape[1]
    full_width = block_width * lax.axis_size("tp")
    width_index = lax.axis_index("tp")
    full_rows = lax.all_gather(tokens, "tp", axis=1, tiled=True)
    full_float = full_rows.astype(jnp.float32)
    normed_full = (
        full_float
        * lax.rsqrt(jnp.mean(full_float * full_float, axis=-1, keepdims=True) + epsilon)
        * norm_gain
    ).astype(jnp.bfloat16)
    normed_block = lax.dynamic_slice_in_dim(normed_full, width_index * block_width, block_width, 1)
    gate_matrix = expert_gate[0]
    up_matrix = expert_up[0]
    down_matrix = expert_down[0]
    experts = lax.axis_size("ep")
    choose = (routes[:, :, None] == jnp.arange(experts, dtype=jnp.int32)[None, None, :]).astype(
        jnp.float32
    )
    weight_table = jnp.sum(route_weights[:, :, None] * choose, axis=1)
    expert_input = lax.all_gather(normed_block, "ep", axis=0, tiled=True)
    table_all = lax.all_gather(weight_table, "ep", axis=0, tiled=True)
    summed = (
        lax.psum(local_product(expert_input, gate_matrix).astype(jnp.bfloat16), "tp").astype(
            jnp.float32
        ),
        lax.psum(local_product(expert_input, up_matrix).astype(jnp.bfloat16), "tp").astype(
            jnp.float32
        ),
        lax.psum(local_product(normed_block, shared_gate).astype(jnp.bfloat16), "tp").astype(
            jnp.float32
        ),
        lax.psum(local_product(normed_block, shared_up).astype(jnp.bfloat16), "tp").astype(
            jnp.float32
        ),
    )
    routed_hidden = (jax.nn.silu(summed[0]) * summed[1]).astype(jnp.bfloat16)
    shared_hidden = (jax.nn.silu(summed[2]) * summed[3]).astype(jnp.bfloat16)
    expert_rows = local_product(routed_hidden, down_matrix).astype(jnp.bfloat16)
    shared_out = local_product(shared_hidden, shared_down)
    own_expert = lax.axis_index("ep")
    column = lax.dynamic_slice_in_dim(table_all, own_expert, 1, 1)
    routed = lax.psum_scatter(
        (column * expert_rows.astype(jnp.float32)).astype(jnp.bfloat16),
        "ep",
        scatter_dimension=0,
        tiled=True,
    ).astype(jnp.float32)
    mixture = routed + shared_out
    square_sum = lax.psum(jnp.sum(mixture * mixture, axis=-1, keepdims=True), "tp")
    scale = lax.rsqrt(square_sum / full_width + epsilon)
    return (mixture * scale * out_gain).astype(jnp.bfloat16)


def solution(mesh):
    chips = mesh.shape["ep"] // 2
    if mesh.shape["tp"] == 2 and mesh.shape["ep"] == 8:
        body = functools.partial(fused, chips)
    else:
        body = per_device
    return jax.shard_map(
        body,
        mesh=mesh,
        in_specs=(
            P(("grp", "ep"), "tp"),
            P(("grp", "ep"), None),
            P(("grp", "ep"), None),
            P(),
            P("ep", "tp", None),
            P("ep", "tp", None),
            P("ep", None, "tp"),
            P("tp", None),
            P("tp", None),
            P(None, "tp"),
            P("tp"),
        ),
        out_specs=P(("grp", "ep"), "tp"),
        check_vma=False,
    )
```

```python
import functools

import jax
import jax.numpy as jnp
from jax import lax
from jax.experimental import pallas as pl
from jax.experimental.pallas import tpu as pltpu
from jax.sharding import PartitionSpec as P

epsilon = 1e-06
MESH = pl.DeviceIdType.MESH
TABLE = 128


def plan(chips):
    ring = [mask for mask in range(2, chips)]
    first = [(0, 0), (0, 1), (1, 0)]
    steps = first + [(mask, 0) for mask in ring] + [(mask, 1) for mask in ring] + [(1, 1), None]
    relays = [[steps.index((distance, 0)), steps.index((max(distance, 2), 1))] for distance in range(1, chips)]
    relays[0][1] -= 1
    return steps, relays


def pick(index, table):
    value = jnp.int32(table[0])
    for position in range(1, len(table)):
        if table[position] != table[0]:
            value = jnp.where(index == position, jnp.int32(table[position]), value)
    return value


def exclusive_or(a, b, size):
    total, unit = jnp.int32(0), 1
    while unit < size:
        total = total + unit * lax.rem(lax.div(a, unit) + lax.div(b, unit), 2)
        unit *= 2
    return total


def fused_kernel(
    chips,
    tokens_hbm,
    routes_hbm,
    weights_hbm,
    norm_gain_hbm,
    gate_hbm,
    up_hbm,
    down_hbm,
    shared_gate_hbm,
    shared_up_hbm,
    shared_down_hbm,
    out_gain_hbm,
    out_ref,
    tokens_ref,
    routes_ref,
    weights_ref,
    norm_gain_ref,
    out_gain_ref,
    gate,
    up,
    down,
    held,
    part_out,
    part_in,
    part_own,
    hidden,
    product,
    waiting,
    pair_out,
    pair_in,
    far_out,
    far_in,
    mixture,
    square_out,
    square_in,
    load_sem,
    square_send,
    square_recv,
    gather_send,
    gather_recv,
    pair_gather_recv,
    part_send,
    part_recv,
    hidden_send,
    hidden_recv,
    pair_send,
    pair_recv,
    far_send,
    far_recv,
):
    rows, width = tokens_ref.shape
    experts = 2 * chips
    units = gate.shape[2]
    half = units // 2
    steps, relays = plan(chips)
    count = len(steps)
    masks = [0 if s is None else s[0] for s in steps]
    lanes = [0 if s is None else s[1] for s in steps]
    shared_at = steps.index(None)

    ep = lax.axis_index("ep")
    tp = lax.axis_index("tp")
    chip, core = lax.div(ep, 2), lax.rem(ep, 2)
    other_core = 1 - core
    partner = {"ep": chip * 2 + other_core}
    across = {"tp": 1 - tp}

    loads = [
        pltpu.make_async_copy(source, target, load_sem.at[i])
        for i, (source, target) in enumerate(
            [
                (gate_hbm.at[0], gate.at[0]),
                (up_hbm.at[0], up.at[0]),
                (shared_gate_hbm, gate.at[1]),
                (shared_up_hbm, up.at[1]),
                (down_hbm.at[0], down.at[0]),
                (shared_down_hbm, down.at[1]),
                (tokens_hbm, tokens_ref),
                (routes_hbm, routes_ref),
                (weights_hbm, weights_ref),
                (norm_gain_hbm, norm_gain_ref),
                (out_gain_hbm, out_gain_ref),
            ]
        )
    ]
    for load in loads[6:] + loads[:2]:
        load.start()

    barrier = pltpu.get_barrier_semaphore()
    for shift in range(1, chips):
        pl.semaphore_signal(
            barrier,
            inc=1,
            device_id={"ep": lax.rem(chip + shift, chips) * 2 + core},
            device_id_type=MESH,
        )
    pl.semaphore_signal(barrier, inc=1, device_id=partner, device_id_type=MESH)
    pl.semaphore_signal(barrier, inc=1, device_id=across, device_id_type=MESH)

    def remote(source, target, send, recv, device):
        return pltpu.make_async_remote_copy(
            src_ref=source,
            dst_ref=target,
            send_sem=send,
            recv_sem=recv,
            device_id=device,
            device_id_type=MESH,
        )

    def square_copy(which):
        return remote(
            square_out.at[which],
            square_in.at[which],
            square_send.at[which],
            square_recv.at[which],
            across,
        )

    def gather_copy(origin, way):
        slot = held.at[origin * 2 + core]
        device = ({"ep": (chip - 1) * 2 + core}, {"ep": (chip + 1) * 2 + core}, partner)[way]
        recv = (pair_gather_recv if way == 2 else gather_recv).at[origin]
        return remote(slot, slot, gather_send.at[origin, way], recv, device)

    def pair_gather_arrival(origin):
        slot = held.at[origin * 2 + other_core]
        return remote(slot, slot, gather_send.at[origin, 2], pair_gather_recv.at[origin], partner)

    def part_copy(k, which):
        return remote(
            part_out.at[k, which],
            part_in.at[k, which],
            part_send.at[k, which],
            part_recv.at[k, which],
            across,
        )

    def hidden_copy(k, side):
        return remote(
            hidden.at[k, side], hidden.at[k, side], hidden_send.at[k], hidden_recv.at[k], across
        )

    def pair_copy(origin):
        return remote(
            pair_out.at[origin],
            pair_in.at[origin],
            pair_send.at[origin],
            pair_recv.at[origin],
            partner,
        )

    beside, opposite, beyond = (exclusive_or(chip, mask, chips) for mask in (1, 2, 3))

    def far_copy(mask, origin):
        slot = jnp.where(mask == 2, beyond, chip)
        return remote(
            far_out.at[origin],
            far_in.at[slot],
            far_send.at[origin],
            far_recv.at[slot],
            {"ep": jnp.where(mask == 3, beyond, beside) * 2 + core},
        )

    def far_arrival(slot):
        return remote(
            far_out.at[slot],
            far_in.at[slot],
            far_send.at[slot],
            far_recv.at[slot],
            {"ep": beside * 2 + core},
        )

    def pack(column):
        return jnp.transpose(jnp.broadcast_to(column, (rows, 128)))[:8]

    def unpack(row):
        return jnp.transpose(jnp.broadcast_to(row[:1], (128, rows)))[:, :1]

    for load in loads[6:]:
        load.wait()
    token_float = tokens_ref[...].astype(jnp.float32)
    own_square = jnp.sum(token_float * token_float, axis=-1, keepdims=True)
    square_out[0] = pack(own_square)
    pl.semaphore_wait(barrier, chips + 1)
    square_copy(0).start()
    lane_ids = lax.broadcasted_iota(jnp.int32, (rows, TABLE), 1)
    expert_ids = lax.broadcasted_iota(jnp.int32, (TABLE, rows), 0)
    table = jnp.zeros((TABLE, rows), jnp.float32)
    for choice in range(routes_ref.shape[0]):
        named = routes_ref[choice : choice + 1, :]
        match = (expert_ids == named) | (expert_ids == named + experts)
        table = table + jnp.where(match, weights_ref[choice : choice + 1, :], 0.0)
    table = jnp.transpose(table)
    coarse = table.astype(jnp.bfloat16).astype(jnp.float32)
    held[ep, :, width:] = jnp.where(lane_ids < experts, table, table - coarse).astype(jnp.bfloat16)
    mixture[...] = jnp.zeros_like(mixture)
    square_copy(0).wait_recv()
    square = own_square + unpack(square_in[0])
    gain = norm_gain_ref[:, pl.ds(pl.multiple_of(tp * width, width), width)]
    held[ep, :, :width] = (
        tokens_ref[...].astype(jnp.float32) * lax.rsqrt(square / (2 * width) + epsilon) * gain
    ).astype(jnp.bfloat16)

    def send_outward():
        @pl.when(chip > 0)
        def _():
            gather_copy(chip, 0).start()

        @pl.when(chip < chips - 1)
        def _():
            gather_copy(chip, 1).start()

    gather_copy(chip, 2).start()
    pl.when(core == 0)(send_outward)

    def locate(k):
        origin = exclusive_or(chip, pick(k, masks), chips)
        lane = pick(k, lanes)
        return origin, lane

    def first_stage(k):
        origin, lane = locate(k)
        is_shared = k == shared_at

        @pl.when(k == 0)
        def _():
            loads[0].wait()
            loads[1].wait()
            for load in loads[2:6]:
                load.start()

        @pl.when(is_shared)
        def _():
            loads[2].wait()
            loads[3].wait()

        for index, positions in enumerate(relays):
            distance = index + 1
            position = jnp.where(core == 0, positions[0], positions[1])

            @pl.when((k == position) & (chip >= distance))
            def _(distance=distance):
                gather_copy(chip - distance, 0).wait_recv()
                gather_copy(chip - distance, 2).start()

                @pl.when(chip < chips - 1)
                def _():
                    gather_copy(chip - distance, 1).start()

            @pl.when((k == position) & (chip + distance < chips))
            def _(distance=distance):
                gather_copy(chip + distance, 1).wait_recv()
                gather_copy(chip + distance, 2).start()

                @pl.when(chip > 0)
                def _():
                    gather_copy(chip + distance, 0).start()

        @pl.when((lane != core) & (k != shared_at))
        def _():
            pair_gather_arrival(origin).wait_recv()

        block = jnp.where(is_shared, ep, origin * 2 + lane)
        kind = jnp.where(is_shared, 1, 0)
        source = held[block, :, :width]
        away = pl.ds(pl.multiple_of((1 - tp) * half, half), half)
        near = pl.ds(pl.multiple_of(tp * half, half), half)
        for which, matrix in enumerate((gate, up)):
            part_out[k, which] = jnp.dot(
                source, matrix[kind, :, away], preferred_element_type=jnp.float32
            ).astype(jnp.bfloat16)
            part_copy(k, which).start()
        for which, matrix in enumerate((gate, up)):
            part_own[k, which] = jnp.dot(
                source, matrix[kind, :, near], preferred_element_type=jnp.float32
            ).astype(jnp.bfloat16)

    def second_stage(k):
        part_copy(k, 0).wait_recv()
        part_copy(k, 1).wait_recv()
        gate_sum = part_own[k, 0].astype(jnp.float32) + part_in[k, 0].astype(jnp.float32)
        up_sum = part_own[k, 1].astype(jnp.float32) + part_in[k, 1].astype(jnp.float32)
        hidden[k, tp] = (jax.nn.silu(gate_sum) * up_sum).astype(jnp.bfloat16)
        hidden_copy(k, tp).start()

    def third_stage(k):
        origin, lane = locate(k)
        is_shared = k == shared_at

        @pl.when(k == 0)
        def _():
            loads[4].wait()
            loads[5].wait()

        hidden_copy(k, 1 - tp).wait_recv()
        block = jnp.where(is_shared, ep, origin * 2 + lane)
        kind = jnp.where(is_shared, 1, 0)
        chosen = (lane_ids == ep) | (lane_ids == ep + experts)
        scale = jnp.sum(
            jnp.where(chosen, held[block, :, width:].astype(jnp.float32), 0.0),
            axis=-1,
            keepdims=True,
        )
        tile = width // 4

        def tile_step(i, carry):
            columns = pl.ds(pl.multiple_of(i * tile, tile), tile)
            product[:, columns] = jnp.dot(
                hidden[k, 0], down[kind, :half, columns], preferred_element_type=jnp.float32
            ) + jnp.dot(
                hidden[k, 1], down[kind, half:, columns], preferred_element_type=jnp.float32
            )
            return carry

        lax.fori_loop(0, 4, tile_step, 0)

        def weighted():
            return product[...].astype(jnp.bfloat16).astype(jnp.float32) * scale

        @pl.when(is_shared)
        def _():
            mixture[...] += product[...]

        @pl.when((k != shared_at) & (lane != core))
        def _():
            pair_out[origin] = weighted().astype(jnp.bfloat16)
            pair_copy(origin).start()

        @pl.when((k != shared_at) & (lane == core))
        def _():
            waiting[...] = weighted()

    def fourth_stage(k):
        origin, lane = locate(k)

        @pl.when((k != shared_at) & (lane == core))
        def _():
            pair_copy(origin).wait_recv()

            @pl.when(origin == chip)
            def _():
                mixture[...] += waiting[...] + pair_in[origin].astype(jnp.float32)

            mask = pick(k, masks)

            @pl.when(mask == 3)
            def _():
                far_arrival(opposite).wait_recv()
                waiting[...] += far_in[opposite].astype(jnp.float32)

            @pl.when(origin != chip)
            def _():
                far_out[origin] = (waiting[...] + pair_in[origin].astype(jnp.float32)).astype(
                    jnp.bfloat16
                )
                far_copy(mask, origin).start()

    def body(i, carry):
        @pl.when(i < count)
        def _():
            first_stage(i)

        @pl.when(i >= 3)
        def _():
            fourth_stage(i - 3)

        @pl.when((i >= 1) & (i < count + 1))
        def _():
            second_stage(i - 1)

        @pl.when((i == 2) & (core == 1))
        def _():
            send_outward()

        @pl.when((i >= 2) & (i < count + 2))
        def _():
            third_stage(i - 2)

        return carry

    lax.fori_loop(0, count + 3, body, 0)

    far_arrival(beside).wait_recv()
    far_arrival(beyond).wait_recv()
    mixture[...] += far_in[beside].astype(jnp.float32) + far_in[beyond].astype(jnp.float32)

    mixed = mixture[...]
    own_total = jnp.sum(mixed * mixed, axis=-1, keepdims=True)
    square_out[1] = pack(own_total)
    square_copy(1).start()
    square_copy(1).wait_recv()
    total = own_total + unpack(square_in[1])
    out_ref[...] = (
        mixture[...] * lax.rsqrt(total / (2 * width) + epsilon) * out_gain_ref[...]
    ).astype(jnp.bfloat16)

    square_copy(0).wait_send()
    square_copy(1).wait_send()
    for origin in range(chips):
        gather_copy(origin, 2).wait_send()
        pair_copy(origin).wait_send()

        @pl.when((chip >= origin) & (chip < chips - 1))
        def _(origin=origin):
            gather_copy(origin, 1).wait_send()

        @pl.when((chip <= origin) & (chip > 0))
        def _(origin=origin):
            gather_copy(origin, 0).wait_send()

        @pl.when(chip != origin)
        def _(origin=origin):
            far_arrival(origin).wait_send()

    def drain(k, carry):
        part_copy(k, 0).wait_send()
        part_copy(k, 1).wait_send()
        hidden_copy(k, tp).wait_send()
        return carry

    lax.fori_loop(0, count, drain, 0)


def fused(
    chips,
    tokens,
    routes,
    route_weights,
    norm_gain,
    expert_gate,
    expert_up,
    expert_down,
    shared_gate,
    shared_up,
    shared_down,
    out_gain,
):
    rows, width = tokens.shape
    units = shared_gate.shape[1]
    half = units // 2
    count = 2 * chips + 1
    choices = routes.shape[1]
    vmem = pl.BlockSpec(memory_space=pltpu.VMEM)
    hbm = pl.BlockSpec(memory_space=pl.ANY)
    bf16, f32 = jnp.bfloat16, jnp.float32
    dma = pltpu.SemaphoreType.DMA
    return pl.pallas_call(
        functools.partial(fused_kernel, chips),
        out_shape=jax.ShapeDtypeStruct((rows, width), bf16),
        in_specs=[hbm] * 11,
        out_specs=vmem,
        scratch_shapes=[
            pltpu.VMEM((rows, width), bf16),
            pltpu.VMEM((choices, rows), jnp.int32),
            pltpu.VMEM((choices, rows), f32),
            pltpu.VMEM((1, norm_gain.shape[0]), f32),
            pltpu.VMEM((1, width), f32),
            pltpu.VMEM((2, width, units), bf16),
            pltpu.VMEM((2, width, units), bf16),
            pltpu.VMEM((2, units, width), bf16),
            pltpu.VMEM((2 * chips, rows, width + TABLE), bf16),
            pltpu.VMEM((count, 2, rows, half), bf16),
            pltpu.VMEM((count, 2, rows, half), bf16),
            pltpu.VMEM((count, 2, rows, half), bf16),
            pltpu.VMEM((count, 2, rows, half), bf16),
            pltpu.VMEM((rows, width), f32),
            pltpu.VMEM((rows, width), f32),
            pltpu.VMEM((chips, rows, width), bf16),
            pltpu.VMEM((chips, rows, width), bf16),
            pltpu.VMEM((chips, rows, width), bf16),
            pltpu.VMEM((chips, rows, width), bf16),
            pltpu.VMEM((rows, width), f32),
            pltpu.VMEM((2, 8, rows), f32),
            pltpu.VMEM((2, 8, rows), f32),
            dma((11,)),
            dma((2,)),
            dma((2,)),
            dma((chips, 3)),
            dma((chips,)),
            dma((chips,)),
            dma((count, 2)),
            dma((count, 2)),
            dma((count,)),
            dma((count,)),
            dma((chips,)),
            dma((chips,)),
            dma((chips,)),
            dma((chips,)),
        ],
        compiler_params=pltpu.CompilerParams(
            collective_id=0, has_side_effects=True, vmem_limit_bytes=60 * 1024 * 1024
        ),
    )(
        tokens,
        routes.T,
        route_weights.T,
        norm_gain.reshape(1, -1),
        expert_gate,
        expert_up,
        expert_down,
        shared_gate,
        shared_up,
        shared_down,
        out_gain.reshape(1, -1),
    )


def local_product(source, matrix):
    return jnp.dot(source, matrix, preferred_element_type=jnp.float32)


def per_device(
    tokens,
    routes,
    route_weights,
    norm_gain,
    expert_gate,
    expert_up,
    expert_down,
    shared_gate,
    shared_up,
    shared_down,
    out_gain,
):
    block_width = tokens.shape[1]
    full_width = block_width * lax.axis_size("tp")
    width_index = lax.axis_index("tp")
    full_rows = lax.all_gather(tokens, "tp", axis=1, tiled=True)
    full_float = full_rows.astype(jnp.float32)
    normed_full = (
        full_float
        * lax.rsqrt(jnp.mean(full_float * full_float, axis=-1, keepdims=True) + epsilon)
        * norm_gain
    ).astype(jnp.bfloat16)
    normed_block = lax.dynamic_slice_in_dim(normed_full, width_index * block_width, block_width, 1)
    gate_matrix = expert_gate[0]
    up_matrix = expert_up[0]
    down_matrix = expert_down[0]
    experts = lax.axis_size("ep")
    choose = (routes[:, :, None] == jnp.arange(experts, dtype=jnp.int32)[None, None, :]).astype(
        jnp.float32
    )
    weight_table = jnp.sum(route_weights[:, :, None] * choose, axis=1)
    expert_input = lax.all_gather(normed_block, "ep", axis=0, tiled=True)
    table_all = lax.all_gather(weight_table, "ep", axis=0, tiled=True)
    summed = (
        lax.psum(local_product(expert_input, gate_matrix).astype(jnp.bfloat16), "tp").astype(
            jnp.float32
        ),
        lax.psum(local_product(expert_input, up_matrix).astype(jnp.bfloat16), "tp").astype(
            jnp.float32
        ),
        lax.psum(local_product(normed_block, shared_gate).astype(jnp.bfloat16), "tp").astype(
            jnp.float32
        ),
        lax.psum(local_product(normed_block, shared_up).astype(jnp.bfloat16), "tp").astype(
            jnp.float32
        ),
    )
    routed_hidden = (jax.nn.silu(summed[0]) * summed[1]).astype(jnp.bfloat16)
    shared_hidden = (jax.nn.silu(summed[2]) * summed[3]).astype(jnp.bfloat16)
    expert_rows = local_product(routed_hidden, down_matrix).astype(jnp.bfloat16)
    shared_out = local_product(shared_hidden, shared_down)
    own_expert = lax.axis_index("ep")
    column = lax.dynamic_slice_in_dim(table_all, own_expert, 1, 1)
    routed = lax.psum_scatter(
        (column * expert_rows.astype(jnp.float32)).astype(jnp.bfloat16),
        "ep",
        scatter_dimension=0,
        tiled=True,
    ).astype(jnp.float32)
    mixture = routed + shared_out
    square_sum = lax.psum(jnp.sum(mixture * mixture, axis=-1, keepdims=True), "tp")
    scale = lax.rsqrt(square_sum / full_width + epsilon)
    return (mixture * scale * out_gain).astype(jnp.bfloat16)


def solution(mesh):
    chips = mesh.shape["ep"] // 2
    if mesh.shape["tp"] == 2 and mesh.shape["ep"] == 8:
        body = functools.partial(fused, chips)
    else:
        body = per_device
    return jax.shard_map(
        body,
        mesh=mesh,
        in_specs=(
            P(("grp", "ep"), "tp"),
            P(("grp", "ep"), None),
            P(("grp", "ep"), None),
            P(),
            P("ep", "tp", None),
            P("ep", "tp", None),
            P("ep", None, "tp"),
            P("tp", None),
            P("tp", None),
            P(None, "tp"),
            P("tp"),
        ),
        out_specs=P(("grp", "ep"), "tp"),
        check_vma=False,
    )
```
